32 devices in a mesh: sp: 16 (over z, y, x), tp: 2 (over core).
Axes of the slice: x: 2, y: 2, z: 4, core: 2. Of those that a mesh axis runs over, the one named last changes fastest.
Arguments:
- resid: bfloat16 [6144, 2048], P('sp', 'tp'), may hold values from -40 to 40
- query_one: bfloat16 [6144, 1024], P('sp', 'tp'), may hold values from -64 to 64
- key_one: bfloat16 [6144, 1024], P('sp', 'tp'), may hold values from -64 to 64
- query_two: bfloat16 [6144, 1024], P('sp', 'tp'), may hold values from -64 to 64
- key_two: bfloat16 [6144, 1024], P('sp', 'tp'), may hold values from -64 to 64
- values: bfloat16 [6144, 2048], P('sp', 'tp'), may hold values from -6 to 6
- mix_lambda: float32 [8], P('tp'), may hold values from 0.3 to 0.8
- segments: int32 [6144], P('sp'), may hold values from 0 to 7, never falling along the last dimension, each value on 1 to 1536 neighbouring positions
- head_gain: float32 [256], replicated, may hold values from 0.1 to 1.9
- out_weight: bfloat16 [2048, 2048], P(None, 'tp'), may hold values from -0.125 to 0.125
- mixer_gain: float32 [2048], P('tp'), may hold values from 0.1 to 1.9
- gate_weight: bfloat16 [2048, 6144], P('sp', 'tp'), may hold values from -0.125 to 0.125
- up_weight: bfloat16 [2048, 6144], P('sp', 'tp'), may hold values from -0.125 to 0.125
- down_weight: bfloat16 [6144, 2048], P('tp', 'sp'), may hold values from -0.078125 to 0.078125
Outputs:
- layer_out: bfloat16 [6144, 2048], P('sp', 'tp')
The draws below stay inside these ranges and needn't reach their ends.
Inputs may be any that keep to these rules, and one draw needn't show every extreme that they name: `segments`: numbers never fall along the sequence; each document has at most 1536 positions and one has exactly that many.
All inputs are finite; a program needn't handle non-finite values.
Results may differ from the reference program's by a relative error of at most 0.012.
Values may be sent and summed in bfloat16 or wider, within the bound.
No kernel may reach another device: no remote copies, remote signals or barrier semaphores. Data moves between devices by JAX's collectives and lax.ppermute only.
A program may use at most 128 MiB of HBM per device.

```python
import math
import jax
import jax.numpy as jnp
import numpy as np
from jax import lax

D = 2048
HEADS = 8
HD = 128
VD = 256
FF = 6144
TOK_DEV = 384
REACH = 4
DOC_MOST = 1536
TOKENS = 6144
DOCS = 8
N_SP = 16
N_TP = 2


def draw_resid(key, part):
    base = jax.random.normal(jax.random.fold_in(key, 11), (TOKENS, D), jnp.float32)
    column = jnp.exp(1.6 * jnp.arange(D, dtype=jnp.float32) / D)
    result = base * column / 2.0
    return jnp.clip(result, -40.0, 40.0).astype(jnp.bfloat16)


def drawn_pair(key, which):
    pair_key = jax.random.fold_in(key, 100 + which)
    width = HEADS * HD
    query = 1.3 * jax.random.normal(jax.random.fold_in(pair_key, 1), (TOKENS, width), jnp.float32)
    keys = 1.3 * jax.random.normal(jax.random.fold_in(pair_key, 2), (TOKENS, width), jnp.float32)
    return (jnp.clip(query, -64.0, 64.0), jnp.clip(keys, -64.0, 64.0))


def draw_query_one(key, part):
    return drawn_pair(key, 1)[0].astype(jnp.bfloat16)


def draw_key_one(key, part):
    return drawn_pair(key, 1)[1].astype(jnp.bfloat16)


def draw_query_two(key, part):
    return drawn_pair(key, 2)[0].astype(jnp.bfloat16)


def draw_key_two(key, part):
    return drawn_pair(key, 2)[1].astype(jnp.bfloat16)


def level_of(own_key, dims, cuts, smallest, largest):
    factor_of = 1.0
    for dim, shards_of in cuts:
        draws = jax.random.uniform(jax.random.fold_in(jax.random.fold_in(own_key, 6), dim), (shards_of,), jnp.float32, smallest / len(cuts), largest / len(cuts))
        factor_of = factor_of * jnp.repeat(jnp.exp(draws), dims[dim] // shards_of).reshape((-1,) + (1,) * (len(dims) - 1 - dim))
    return factor_of


def length_profile(number_of, total, bound, lean):
    weights = [(1 << 20) // math.isqrt(grade ** lean) + 1 for grade in range(2, number_of + 1)]
    rest, counts = total - bound - (number_of - 1), [1] * (number_of - 1)
    while rest > 0:
        movable = [i for i in range(number_of - 1) if counts[i] < bound]
        pool, left = sum([weights[i] for i in movable]), rest
        for i in movable:
            addition = min(bound - counts[i], max(1, left * weights[i] // pool), rest)
            counts[i] = counts[i] + addition
            rest = rest - addition
    return np.array([bound] + counts)


def uneven_parts(rng, count, total, limit, slope):
    if count == 2:
        one = jax.random.randint(rng, (), max(1, total - limit), min(limit, total - 1) + 1)
        return jnp.stack([one, total - one])
    sizes = jnp.asarray(length_profile(count, total, limit, slope), jnp.int32)
    pairs = (count - 1) // 2
    giver, receiver = sizes[1:1 + 2 * pairs:2], sizes[2:2 + 2 * pairs:2]
    slack = jnp.minimum(giver - 1, limit - receiver)
    moved = jax.random.randint(jax.random.fold_in(rng, 1), (pairs,), 0, 1 << 20) % (slack + 1)
    sizes = sizes.at[1:1 + 2 * pairs:2].set(giver - moved).at[2:2 + 2 * pairs:2].set(receiver + moved)
    return sizes[jax.random.permutation(jax.random.fold_in(rng, 2), count)]


def normal_values(stream_key, dims, scale, reach, split=(), kind=jnp.bfloat16):
    values = jax.random.normal(stream_key, dims, jnp.float32) * scale
    if len(split) > 0:
        values = level_of(stream_key, dims, split, -0.22, 0.18) * values
    return jnp.clip(values, min=-reach, max=reach).astype(kind)


def setup_inputs(seed: int = 0) -> dict:
    arg_keys = jax.random.split(jax.random.key(seed), 15)
    resid = draw_resid(jax.random.fold_in(arg_keys[14], 71), 0)
    query_one = draw_query_one(jax.random.fold_in(arg_keys[14], 71), 0)
    key_one = draw_key_one(jax.random.fold_in(arg_keys[14], 71), 0)
    query_two = draw_query_two(jax.random.fold_in(arg_keys[14], 71), 0)
    key_two = draw_key_two(jax.random.fold_in(arg_keys[14], 71), 0)
    values = normal_values(arg_keys[5], (TOKENS, HEADS * VD), 1.0, 6.0, ((0, 16), (1, 2)))
    mix_lambda = jnp.clip(0.3 + 0.5 * jax.random.uniform(arg_keys[6], (HEADS,), jnp.float32) ** level_of(arg_keys[6], (HEADS,), ((0, 2),), -0.2, 0.2), 0.3, 0.8)
    segments = jnp.searchsorted(jnp.cumsum(uneven_parts(arg_keys[7], DOCS, TOKENS, DOC_MOST, 0)), jnp.arange(TOKENS), side="right").astype(jnp.int32)
    head_gain = jnp.clip(1.0 + 0.18 * jax.random.normal(arg_keys[8], (VD,), jnp.float32), 0.1, 1.9)
    out_weight = normal_values(arg_keys[9], (HEADS * VD, D), (HEADS * VD) ** -0.5, 0.125, ((1, 2),))
    mixer_gain = jnp.clip(1.0 + 0.18 * jax.random.normal(arg_keys[10], (D,), jnp.float32), 0.1, 1.9)
    gate_weight = normal_values(arg_keys[11], (D, FF), D ** -0.5, 0.125, ((0, 16), (1, 2)))
    up_weight = normal_values(arg_keys[12], (D, FF), D ** -0.5, 0.125, ((0, 16), (1, 2)))
    down_weight = normal_values(arg_keys[13], (FF, D), FF ** -0.5, 0.078125, ((0, 2), (1, 16)))
    return {"resid": resid, "query_one": query_one, "key_one": key_one, "query_two": query_two, "key_two": key_two, "values": values, "mix_lambda": mix_lambda, "segments": segments, "head_gain": head_gain, "out_weight": out_weight, "mixer_gain": mixer_gain, "gate_weight": gate_weight, "up_weight": up_weight, "down_weight": down_weight}


def reference(resid, query_one, key_one, query_two, key_two, values, mix_lambda, segments, head_gain, out_weight, mixer_gain, gate_weight, up_weight, down_weight):
    rows = TOK_DEV
    span = REACH * TOK_DEV

    def padded(array):
        return jnp.concatenate([jnp.zeros((span,) + array.shape[1:], array.dtype), array], 0)
    key_first = padded(key_one)
    key_second = padded(key_two)
    value_pad = padded(values)
    seg_pad = jnp.concatenate([jnp.full((span,), -1, jnp.int32), segments.astype(jnp.int32)], 0)

    def block(index):
        start = (index * rows).astype(jnp.int32)
        width = span + rows
        q_first = lax.dynamic_slice_in_dim(query_one, start, rows, 0).reshape(rows, HEADS, HD).astype(jnp.float32)
        q_second = lax.dynamic_slice_in_dim(query_two, start, rows, 0).reshape(rows, HEADS, HD).astype(jnp.float32)
        k_first = lax.dynamic_slice_in_dim(key_first, start, width, 0).reshape(width, HEADS, HD).astype(jnp.float32)
        k_second = lax.dynamic_slice_in_dim(key_second, start, width, 0).reshape(width, HEADS, HD).astype(jnp.float32)
        vals = lax.dynamic_slice_in_dim(value_pad, start, width, 0).reshape(width, HEADS, VD).astype(jnp.float32)
        seg_query = lax.dynamic_slice_in_dim(segments.astype(jnp.int32), start, rows, 0)
        seg_key = lax.dynamic_slice_in_dim(seg_pad, start, width, 0)
        q_pos = start + jnp.arange(rows, dtype=jnp.int32)
        k_pos = start - span + jnp.arange(width, dtype=jnp.int32)
        allowed = (seg_key[None, :] == seg_query[:, None]) & (k_pos[None, :] <= q_pos[:, None]) & (k_pos[None, :] >= 0)

        def weights(query, keys):
            score = jnp.einsum('qhd,khd->hqk', query, keys) * HD ** (-0.5)
            score = jnp.where(allowed[None], score, -jnp.inf)
            score = score - lax.optimization_barrier(jnp.max(score, axis=-1, keepdims=True))
            expo = jnp.exp(score)
            return (expo / lax.optimization_barrier(jnp.sum(expo, axis=-1, keepdims=True))).astype(jnp.bfloat16)
        probs_first = weights(q_first, k_first).astype(jnp.float32)
        probs_second = weights(q_second, k_second).astype(jnp.float32)
        out_first = jnp.einsum('hqk,khe->qhe', probs_first, vals)
        out_second = jnp.einsum('hqk,khe->qhe', probs_second, vals)
        head_out = out_first - mix_lambda[None, :, None] * out_second
        meansq = lax.optimization_barrier(jnp.mean(head_out * head_out, axis=-1, keepdims=True))
        normal = head_out * lax.rsqrt(meansq + 1e-05) * head_gain
        return normal.reshape(rows, HEADS * VD).astype(jnp.bfloat16)
    attn_rows = lax.map(block, jnp.arange(N_SP, dtype=jnp.int32)).reshape(TOKENS, HEADS * VD)
    mid = (resid.astype(jnp.float32) + jnp.dot(attn_rows, out_weight, preferred_element_type=jnp.float32)).astype(jnp.bfloat16)
    midf = mid.astype(jnp.float32)
    meansq = lax.optimization_barrier(jnp.mean(midf * midf, axis=-1, keepdims=True))
    normed = (midf * lax.rsqrt(meansq + 1e-06) * mixer_gain).astype(jnp.bfloat16)
    gate = jnp.dot(normed, gate_weight, preferred_element_type=jnp.float32)
    up = jnp.dot(normed, up_weight, preferred_element_type=jnp.float32)
    hidden = (jax.nn.silu(gate) * up).astype(jnp.bfloat16)
    blocks = FF // N_TP
    hidden_blocks = hidden.reshape(TOKENS, N_TP, blocks).transpose(1, 0, 2)
    down_blocks = down_weight.reshape(N_TP, blocks, D)

    def add_block(total, pair):
        part = jnp.dot(pair[0], pair[1], preferred_element_type=jnp.float32).astype(jnp.bfloat16)
        part = lax.optimization_barrier(part)
        return (total + part.astype(jnp.float32), None)
    summed, unused = lax.scan(add_block, jnp.zeros((TOKENS, D), jnp.float32), (hidden_blocks, down_blocks))
    return (midf + summed).astype(jnp.bfloat16)
```

```python
import math

import jax
import jax.numpy as jnp
from jax import lax
from jax.experimental import pallas as pl
from jax.experimental.pallas import tpu as pltpu
from jax.sharding import Mesh, PartitionSpec as P

HD = 128
VD = 256
REACH = 4
QB = 128


def swap(value):
    return lax.ppermute(value, "tp", [(0, 1), (1, 0)])


def tp_gather(value, axis):
    if lax.axis_size("tp") != 2:
        return lax.all_gather(value, "tp", axis=axis, tiled=True)
    other = swap(value)
    first = lax.axis_index("tp") == 0
    return jnp.concatenate(
        [jnp.where(first, value, other), jnp.where(first, other, value)], axis
    )


def tp_sum(value):
    if lax.axis_size("tp") != 2:
        return lax.psum(value, "tp")
    return value + swap(value)


def tp_reduce_scatter(value):
    if lax.axis_size("tp") != 2:
        return lax.psum_scatter(value, "tp", scatter_dimension=1, tiled=True).astype(jnp.float32)
    half = value.shape[1] // 2
    me = lax.axis_index("tp")
    mine = lax.dynamic_slice_in_dim(value, me * half, half, 1)
    theirs = lax.dynamic_slice_in_dim(value, (1 - me) * half, half, 1)
    return mine.astype(jnp.float32) + swap(theirs).astype(jnp.float32)


def shift(value, axis, by):
    length = lax.axis_size(axis)
    return lax.ppermute(value, axis, [(i, (i + by) % length) for i in range(length)])


def attention_kernel(lam_ref, q_ref, kv_prev_ref, kv_ref, seg_q_ref, seg_k_ref, gain_ref, out_ref, kv_all):
    step = pl.program_id(1)
    rows = kv_ref.shape[1]
    span = kv_prev_ref.shape[1]

    @pl.when(step == 0)
    def _():
        kv_all[:span] = kv_prev_ref[0]
        kv_all[span:] = kv_ref[0]

    width = span + QB
    start = pl.multiple_of(step * QB, QB)
    seg_q = seg_q_ref[...]
    seg_k = seg_k_ref[:, pl.ds(start, width)]
    q_pos = lax.broadcasted_iota(jnp.int32, (QB, 1), 0) + span
    k_pos = lax.broadcasted_iota(jnp.int32, (1, width), 1)
    allowed = (seg_k == seg_q) & (k_pos <= q_pos)
    vals = kv_all[pl.ds(start, width), 2 * HD :]

    def one(which):
        query = q_ref[0, :, which * HD : (which + 1) * HD]
        keys = kv_all[pl.ds(start, width), which * HD : (which + 1) * HD]
        score = lax.dot_general(
            query, keys, (((1,), (1,)), ((), ())), preferred_element_type=jnp.float32
        )
        score = jnp.where(allowed, score * HD ** (-0.5), -1e30)
        score = score - jnp.max(score, axis=-1, keepdims=True)
        expo = jnp.exp(score)
        total = jnp.sum(expo, axis=-1, keepdims=True)
        probs = (expo * (1.0 / total)).astype(jnp.bfloat16)
        return jnp.dot(probs, vals, preferred_element_type=jnp.float32)

    head_out = one(0) - lam_ref[pl.program_id(0)] * one(1)
    meansq = jnp.mean(head_out * head_out, axis=-1, keepdims=True)
    out_ref[0] = (head_out * lax.rsqrt(meansq + 1e-05) * gain_ref[...]).astype(jnp.bfloat16)


def attention(query, kv_prev, kv, lam, seg_q, seg_k, gain):
    heads, rows, _ = query.shape
    span = kv_prev.shape[1]
    wide = 2 * HD + VD
    return pl.pallas_call(
        attention_kernel,
        grid=(heads, rows // QB),
        in_specs=[
            pl.BlockSpec(memory_space=pltpu.SMEM),
            pl.BlockSpec((1, QB, 2 * HD), lambda h, i: (h, i, 0)),
            pl.BlockSpec((1, span, wide), lambda h, i: (h, 0, 0)),
            pl.BlockSpec((1, rows, wide), lambda h, i: (h, 0, 0)),
            pl.BlockSpec((QB, 1), lambda h, i: (i, 0)),
            pl.BlockSpec((1, span + rows), lambda h, i: (0, 0)),
            pl.BlockSpec((1, VD), lambda h, i: (0, 0)),
        ],
        out_specs=pl.BlockSpec((1, QB, VD), lambda h, i: (h, i, 0)),
        out_shape=jax.ShapeDtypeStruct((heads, rows, VD), jnp.bfloat16),
        scratch_shapes=[pltpu.VMEM((span + rows, wide), jnp.bfloat16)],
        compiler_params=pltpu.CompilerParams(
            dimension_semantics=("arbitrary", "arbitrary"), vmem_limit_bytes=48 * 2**20
        ),
        cost_estimate=pl.CostEstimate(
            flops=heads * rows * (span + QB) * (2 * HD + 2 * VD) * 2,
            bytes_accessed=heads * (span + 3 * rows) * wide * 2,
            transcendentals=heads * rows * (span + QB) * 2,
        ),
        name="diff_attention",
    )(lam, query, kv_prev, kv, seg_q, seg_k, gain)


def body(
    resid,
    query_one,
    key_one,
    query_two,
    key_two,
    values,
    mix_lambda,
    segments,
    head_gain,
    out_weight,
    mixer_gain,
    gate_weight,
    up_weight,
    down_weight,
):
    rows = query_one.shape[0]
    heads = mix_lambda.shape[0]
    group = lax.axis_size("sg")
    planes = lax.axis_size("sz")
    plane = lax.axis_index("sz")
    member = lax.axis_index("sg")
    hidden = gate_weight.shape[1] // group
    krows = gate_weight.shape[0]
    dcols = down_weight.shape[1]

    gate_up = jnp.concatenate(
        [gate_weight.reshape(krows, group, hidden), up_weight.reshape(krows, group, hidden)], 2
    ).transpose(1, 0, 2)
    gate_up = lax.all_to_all(gate_up, "sg", 0, 0, tiled=True).reshape(group * krows, 2 * hidden)

    kv = jnp.concatenate(
        [
            key_one.reshape(rows, heads, HD),
            key_two.reshape(rows, heads, HD),
            values.reshape(rows, heads, VD),
        ],
        2,
    ).transpose(1, 0, 2)
    query = jnp.concatenate(
        [query_one.reshape(rows, heads, HD), query_two.reshape(rows, heads, HD)], 2
    ).transpose(1, 0, 2)
    gate_up, kv = lax.optimization_barrier((gate_up, kv))
    gate_up = lax.all_gather(gate_up, "sz", axis=0, tiled=True)
    seg_all = lax.all_gather(segments, ("sz", "sg"), axis=0, tiled=True)
    gain = head_gain.reshape(1, VD)
    ahead = [(i, i + 1) for i in range(planes - 1)]

    split = heads % group == 0 and group >= REACH
    if split:
        each = heads // group
        span = REACH * rows
        whole = group * rows

        def to_heads(x):
            x = lax.all_to_all(x.reshape(group, each, rows, -1), "sg", 0, 0, tiled=True)
            return x.transpose(1, 0, 2, 3).reshape(each, whole, -1)

        kv = to_heads(kv)
        kv_prev = lax.ppermute(kv[:, whole - span :], "sz", ahead)
        kv_barred, query = lax.optimization_barrier((kv, query))
        query = to_heads(query)
        lam = lax.dynamic_slice_in_dim(mix_lambda, member * each, each, 0)
        first = plane * whole
    else:
        span = REACH * rows
        whole = rows
        count = group * planes
        lam = mix_lambda
        pieces = [
            lax.ppermute(kv, ("sz", "sg"), [(i, i + by) for i in range(count - by)])
            for by in range(REACH, 0, -1)
        ]
        kv_prev = jnp.concatenate(pieces, 1)
        first = (plane * group + member) * rows

    seg_pad = jnp.concatenate([jnp.full((span,), -1, jnp.int32), seg_all.astype(jnp.int32)])
    seg_k = lax.dynamic_slice_in_dim(seg_pad, first, span + whole, 0)
    seg_q = seg_k[span:].reshape(whole, 1)
    attn = attention(query, kv_prev, kv, lam, seg_q, seg_k.reshape(1, span + whole), gain)

    down = down_weight.reshape(group, hidden, dcols)
    down, query_done = lax.optimization_barrier((down, query))
    down = lax.all_to_all(down, "sg", 0, 0, tiled=True)
    down = lax.all_gather(down, "sz", axis=0, tiled=True)

    if split:
        back = attn.reshape(each, group, rows, VD).transpose(1, 0, 2, 3)
        back = lax.all_to_all(back, "sg", 0, 0, tiled=True).reshape(heads, rows, VD)
    else:
        back = attn
    attn_rows = back.transpose(1, 0, 2).reshape(rows, heads * VD)
    projected = jnp.dot(tp_gather(attn_rows, 1), out_weight, preferred_element_type=jnp.float32)
    mid = (resid.astype(jnp.float32) + projected).astype(jnp.bfloat16)
    midf = mid.astype(jnp.float32)
    squares = tp_sum(jnp.sum(midf * midf, axis=1))
    channels = mid.shape[1] * lax.axis_size("tp")
    normed = (midf * lax.rsqrt(squares / channels + 1e-06)[:, None] * mixer_gain).astype(
        jnp.bfloat16
    )

    blocks = [normed] + [shift(normed, "sg", by) for by in range(1, group)]
    whole_rows = tp_gather(jnp.concatenate(blocks, 0), 1)
    both = jnp.dot(whole_rows, gate_up, preferred_element_type=jnp.float32)
    act = (jax.nn.silu(both[:, :hidden]) * both[:, hidden:]).astype(jnp.bfloat16)
    down_full = down.transpose(1, 0, 2).reshape(hidden, planes * group * dcols)
    terms = jnp.dot(act, down_full, preferred_element_type=jnp.float32).astype(jnp.bfloat16)
    part = tp_reduce_scatter(terms)
    total = part[:rows]
    send = part.astype(jnp.bfloat16)
    for by in range(1, group):
        total = total + shift(send[by * rows : (by + 1) * rows], "sg", -by).astype(jnp.float32)
    return (midf + total).astype(jnp.bfloat16)


def solution(mesh):
    count, cores = mesh.shape["sp"], mesh.shape["tp"]
    group = math.gcd(count, REACH)
    grid = Mesh(mesh.devices.reshape(count // group, group, cores), ("sz", "sg", "tp"))
    sp = ("sz", "sg")
    in_specs = (
        P(sp, "tp"),
        P(sp, "tp"),
        P(sp, "tp"),
        P(sp, "tp"),
        P(sp, "tp"),
        P(sp, "tp"),
        P("tp"),
        P(sp),
        P(),
        P(None, "tp"),
        P("tp"),
        P(sp, "tp"),
        P(sp, "tp"),
        P("tp", sp),
    )
    return jax.shard_map(
        body, mesh=grid, in_specs=in_specs, out_specs=P(sp, "tp"), check_vma=False
    )
```

```python
import math

import jax
import jax.numpy as jnp
from jax import lax
from jax.experimental import pallas as pl
from jax.experimental.pallas import tpu as pltpu
from jax.sharding import Mesh, PartitionSpec as P

HD = 128
VD = 256
REACH = 4
QB = 128


def swap(value):
    return lax.ppermute(value, "tp", [(0, 1), (1, 0)])


def halves(weight, axis):
    if lax.axis_size("tp") != 2:
        return (weight, None)
    half = weight.shape[axis] // 2
    me = lax.axis_index("tp")
    return (
        lax.dynamic_slice_in_dim(weight, me * half, half, axis),
        lax.dynamic_slice_in_dim(weight, (1 - me) * half, half, axis),
    )


def tp_dot(value, parts):
    if parts[1] is None:
        value = lax.all_gather(value, "tp", axis=1, tiled=True)
        return jnp.dot(value, parts[0], preferred_element_type=jnp.float32)
    other = swap(value)
    return jnp.dot(value, parts[0], preferred_element_type=jnp.float32) + jnp.dot(
        other, parts[1], preferred_element_type=jnp.float32
    )


def dot_scatter(value, parts):
    if parts[1] is None:
        terms = jnp.dot(value, parts[0], preferred_element_type=jnp.float32).astype(jnp.bfloat16)
        terms = lax.psum_scatter(terms, "tp", scatter_dimension=1, tiled=True)
        return terms.astype(jnp.float32)
    away = jnp.dot(value, parts[1], preferred_element_type=jnp.float32).astype(jnp.bfloat16)
    came = swap(away).astype(jnp.float32)
    return jnp.dot(value, parts[0], preferred_element_type=jnp.float32) + came


def tp_sum(value):
    if lax.axis_size("tp") != 2:
        return lax.psum(value, "tp")
    return value + swap(value)


def mirrored(value, by):
    if by == 0:
        return value
    return lax.ppermute(value, "sg", [(i, i ^ by) for i in range(lax.axis_size("sg"))])


def attention_kernel(lam_ref, q_ref, kv_prev_ref, kv_ref, seg_q_ref, seg_k_ref, gain_ref, out_ref, kv_all):
    step = pl.program_id(1)
    span = kv_prev_ref.shape[1]

    @pl.when(step == 0)
    def _():
        kv_all[:span] = kv_prev_ref[0]
        kv_all[span:] = kv_ref[0]

    width = span + QB
    start = pl.multiple_of(step * QB, QB)
    seg_q = seg_q_ref[...]
    seg_k = seg_k_ref[:, pl.ds(start, width)]
    q_pos = lax.broadcasted_iota(jnp.int32, (QB, 1), 0) + span
    k_pos = lax.broadcasted_iota(jnp.int32, (1, width), 1)
    allowed = (seg_k == seg_q) & (k_pos <= q_pos)
    vals = kv_all[pl.ds(start, width), 2 * HD :]

    def one(which):
        query = q_ref[0, :, which * HD : (which + 1) * HD]
        keys = kv_all[pl.ds(start, width), which * HD : (which + 1) * HD]
        score = lax.dot_general(
            query, keys, (((1,), (1,)), ((), ())), preferred_element_type=jnp.float32
        )
        score = jnp.where(allowed, score * HD ** (-0.5), -1e30)
        score = score - jnp.max(score, axis=-1, keepdims=True)
        expo = jnp.exp(score)
        total = jnp.sum(expo, axis=-1, keepdims=True)
        probs = (expo * (1.0 / total)).astype(jnp.bfloat16)
        return jnp.dot(probs, vals, preferred_element_type=jnp.float32)

    head_out = one(0) - lam_ref[pl.program_id(0)] * one(1)
    meansq = jnp.mean(head_out * head_out, axis=-1, keepdims=True)
    out_ref[0] = (head_out * lax.rsqrt(meansq + 1e-05) * gain_ref[...]).astype(jnp.bfloat16)


def attention(query, kv_prev, kv, lam, seg_q, seg_k, gain):
    heads, rows, _ = query.shape
    span = kv_prev.shape[1]
    wide = 2 * HD + VD
    return pl.pallas_call(
        attention_kernel,
        grid=(heads, rows // QB),
        in_specs=[
            pl.BlockSpec(memory_space=pltpu.SMEM),
            pl.BlockSpec((1, QB, 2 * HD), lambda h, i: (h, i, 0)),
            pl.BlockSpec((1, span, wide), lambda h, i: (h, 0, 0)),
            pl.BlockSpec((1, rows, wide), lambda h, i: (h, 0, 0)),
            pl.BlockSpec((QB, 1), lambda h, i: (i, 0)),
            pl.BlockSpec((1, span + rows), lambda h, i: (0, 0)),
            pl.BlockSpec((1, VD), lambda h, i: (0, 0)),
        ],
        out_specs=pl.BlockSpec((1, QB, VD), lambda h, i: (h, i, 0)),
        out_shape=jax.ShapeDtypeStruct((heads, rows, VD), jnp.bfloat16),
        scratch_shapes=[pltpu.VMEM((span + rows, wide), jnp.bfloat16)],
        compiler_params=pltpu.CompilerParams(
            dimension_semantics=("arbitrary", "arbitrary"), vmem_limit_bytes=48 * 2**20
        ),
        cost_estimate=pl.CostEstimate(
            flops=heads * rows * (span + QB) * (2 * HD + 2 * VD) * 2,
            bytes_accessed=heads * (span + 3 * rows) * wide * 2,
            transcendentals=heads * rows * (span + QB) * 2,
        ),
        name="diff_attention",
    )(lam, query, kv_prev, kv, seg_q, seg_k, gain)


def body(
    resid,
    query_one,
    key_one,
    query_two,
    key_two,
    values,
    mix_lambda,
    segments,
    head_gain,
    out_weight,
    mixer_gain,
    gate_weight,
    up_weight,
    down_weight,
):
    rows = query_one.shape[0]
    heads = mix_lambda.shape[0]
    group = lax.axis_size("sg")
    member = lax.axis_index("sg")
    hidden = gate_weight.shape[1] // group
    krows = gate_weight.shape[0]
    dcols = down_weight.shape[1]

    planes = lax.axis_size("sz")
    ahead = [(i, i + 1) for i in range(planes - 1)]
    seg_here = lax.all_gather(segments.astype(jnp.int32) + 1, "sg", axis=0, tiled=True)
    seg_here, gate_weight = lax.optimization_barrier((seg_here, gate_weight))
    seg_back = lax.ppermute(seg_here, "sz", ahead)
    gate_up = jnp.concatenate(
        [gate_weight.reshape(krows, group, hidden), up_weight.reshape(krows, group, hidden)], 2
    ).transpose(1, 0, 2)
    gate_up = lax.all_to_all(gate_up, "sg", 0, 0, tiled=True).reshape(group * krows, 2 * hidden)

    kv = jnp.concatenate(
        [
            key_one.reshape(rows, heads, HD),
            key_two.reshape(rows, heads, HD),
            values.reshape(rows, heads, VD),
        ],
        2,
    ).transpose(1, 0, 2)
    query = jnp.concatenate(
        [query_one.reshape(rows, heads, HD), query_two.reshape(rows, heads, HD)], 2
    ).transpose(1, 0, 2)
    gate_up, kv = lax.optimization_barrier((gate_up, kv))
    gate_up = lax.all_gather(gate_up, "sz", axis=0, tiled=True)
    gain = head_gain.reshape(1, VD)

    split = heads % group == 0 and group >= REACH
    if split:
        each = heads // group
        span = REACH * rows
        whole = group * rows

        def to_heads(x):
            x = lax.all_to_all(x.reshape(group, each, rows, -1), "sg", 0, 0, tiled=True)
            return x.transpose(1, 0, 2, 3).reshape(each, whole, -1)

        kv = to_heads(kv)
        kv_prev = lax.ppermute(kv[:, whole - span :], "sz", ahead)
        kv, query = lax.optimization_barrier((kv, query))
        query = to_heads(query)
        lam = lax.dynamic_slice_in_dim(mix_lambda, member * each, each, 0)
        first = group * rows - span
    else:
        span = REACH * rows
        whole = rows
        count = group * planes
        lam = mix_lambda
        pieces = [
            lax.ppermute(kv, ("sz", "sg"), [(i, i + by) for i in range(count - by)])
            for by in range(REACH, 0, -1)
        ]
        kv_prev = jnp.concatenate(pieces, 1)
        first = (group + member) * rows - span

    seg_both = jnp.concatenate([seg_back, seg_here])
    seg_k = lax.dynamic_slice_in_dim(seg_both, first, span + whole, 0)
    seg_q = seg_k[span:].reshape(whole, 1)
    attn = attention(query, kv_prev, kv, lam, seg_q, seg_k.reshape(1, span + whole), gain)

    down = down_weight.T.reshape(dcols, group, hidden).transpose(1, 0, 2)
    down, _ = lax.optimization_barrier((down, query))
    down = lax.all_to_all(down, "sg", 0, 0, tiled=True).reshape(group * dcols, hidden)
    down = lax.all_gather(down, "sz", axis=0, tiled=True)

    if split:
        back = attn.reshape(each, group, rows, VD).transpose(1, 0, 2, 3)
        back = lax.all_to_all(back, "sg", 0, 0, tiled=True).reshape(heads, rows, VD)
    else:
        back = attn
    attn_rows = back.transpose(1, 0, 2).reshape(rows, heads * VD)
    projected = tp_dot(attn_rows, halves(out_weight, 0))
    mid = (resid.astype(jnp.float32) + projected).astype(jnp.bfloat16)
    midf = mid.astype(jnp.float32)
    squares = tp_sum(jnp.sum(midf * midf, axis=1))
    channels = mid.shape[1] * lax.axis_size("tp")
    normed = (midf * lax.rsqrt(squares / channels + 1e-06)[:, None] * mixer_gain).astype(
        jnp.bfloat16
    )

    blocks = [mirrored(normed, by) for by in range(group)]
    gate_up_parts = halves(gate_up, 0)
    down_parts = [None if part is None else part.T for part in halves(down, 0)]
    total = jnp.zeros(normed.shape, jnp.float32)
    for first_by, last_by in [(0, 1), (1, 3), (3, 4)]:
        chosen = list(range(first_by, min(last_by, group)))
        if not chosen:
            continue
        together = jnp.concatenate([blocks[by] for by in chosen], 0)
        both = tp_dot(together, gate_up_parts)
        act = (jax.nn.silu(both[:, :hidden]) * both[:, hidden:]).astype(jnp.bfloat16)
        part = dot_scatter(act, down_parts)
        for spot, by in enumerate(chosen):
            piece = part[spot * rows : (spot + 1) * rows]
            if by:
                piece = mirrored(piece.astype(jnp.bfloat16), by).astype(jnp.float32)
            total = total + piece
    return (midf + total).astype(jnp.bfloat16)


def solution(mesh):
    count, cores = mesh.shape["sp"], mesh.shape["tp"]
    group = math.gcd(count, REACH)
    grid = Mesh(mesh.devices.reshape(count // group, group, cores), ("sz", "sg", "tp"))
    sp = ("sz", "sg")
    in_specs = (
        P(sp, "tp"),
        P(sp, "tp"),
        P(sp, "tp"),
        P(sp, "tp"),
        P(sp, "tp"),
        P(sp, "tp"),
        P("tp"),
        P(sp),
        P(),
        P(None, "tp"),
        P("tp"),
        P(sp, "tp"),
        P(sp, "tp"),
        P("tp", sp),
    )

    return jax.shard_map(body, mesh=grid, in_specs=in_specs, out_specs=P(sp, "tp"), check_vma=False)
```
